32 devices in a mesh: sp: 4 (over y, x), tp: 8 (over z, core).
Axes of the slice: x: 2, y: 2, z: 4, core: 2. Of those that a mesh axis runs over, the one named last changes fastest.
Arguments:
- gate_b: bfloat16 [2048, 1024], P('sp', 'tp'), may hold values from -6 to 6
- gate_c: bfloat16 [2048, 1024], P('sp', 'tp'), may hold values from -6 to 6
- values_in: bfloat16 [2048, 1024], P('sp', 'tp'), may hold values from -6 to 6
- conv_w: bfloat16 [3, 1024], P(None, 'tp'), may hold values from -3.5 to 3.5
- documents: int32 [2048], P('sp'), may hold values from 0 to 2, never falling along the last dimension, each value on 1 to 1024 neighbouring positions
- w_out: bfloat16 [1024, 2048], replicated, may hold values from -0.1875 to 0.1875
- resid: bfloat16 [2048, 2048], P(('sp', 'tp')), may hold values from -6 to 6
- norm_gain: bfloat16 [2048], replicated, may hold values from 0.099609375 to 1.8984375
- route_ids: int32 [2048, 2], P(('sp', 'tp')), may hold values from 0 to 3, all different within a row; in each aligned block of 64 rows (0 to 63, 64 to 127, ...) at most 64 rows name the same one
- route_weight: float32 [2048, 2], P(('sp', 'tp')), may hold values from 0.2 to 1
- w_gate: bfloat16 [4, 2048, 7168], P('sp', None, 'tp'), may hold values from -0.125 to 0.125
- w_up: bfloat16 [4, 2048, 7168], P('sp', None, 'tp'), may hold values from -0.125 to 0.125
- w_down: bfloat16 [4, 7168, 2048], P('sp', 'tp'), may hold values from -0.0625 to 0.0625
Outputs:
- layer_out: bfloat16 [2048, 2048], P(('sp', 'tp'))
The draws below stay inside these ranges and needn't reach their ends.
Inputs may be any that keep to these rules, and one draw needn't show every extreme that they name: `route_ids`: each token names two different experts; in the rows of one device no expert is named by more than 64 rows, a bound that some block reaches. `documents`: document numbers never fall along the positions; a document has at most 2048 // 2 positions.
All inputs are finite; a program needn't handle non-finite values.
Results may differ from the reference program's by a relative error of at most 0.018.
Values may be sent and summed in bfloat16 or wider, within the bound.
A program may use at most 128 MiB of HBM per device.

```python
import math
import jax
import jax.numpy as jnp
import numpy as np
from jax import lax

D = 2048
CH = 1024
FF_E = 7168
KW = 3
TOKENS = 2048
ROWS = 64
EXPERTS = 4
CAP = 64
N_SP = 4
N_TP = 8


def shard_levels(key, extent, cuts, least, high):
    gain, own = 1.0, jax.random.fold_in(key, 6)
    for dim, shards_of in cuts:
        draws = jnp.exp(jax.random.uniform(jax.random.fold_in(own, dim), (shards_of,), jnp.float32, least / len(cuts), high / len(cuts)))
        gain = gain * jnp.repeat(draws, extent[dim] // shards_of).reshape([-1 if axis == dim else 1 for axis in range(len(extent))])
    return gain


def profile(number_of, total, bound, skew):
    portions = [(1 << 20) // math.isqrt(rank ** skew) + 1 for rank in range(2, number_of + 1)]
    surplus, counts = total - bound - (number_of - 1), [1] * (number_of - 1)
    while surplus > 0:
        candidates = [i for i in range(number_of - 1) if counts[i] < bound]
        mass, left = sum([portions[i] for i in candidates]), surplus
        for i in candidates:
            addition = min(bound - counts[i], max(1, left * portions[i] // mass), surplus)
            counts[i] = counts[i] + addition
            surplus = surplus - addition
    return np.array([bound] + counts)


def ragged_sizes(stream_key, amount, total, limit, skew):
    if amount == 2:
        one = jax.random.randint(stream_key, (), max(1, total - limit), min(limit, total - 1) + 1)
        return jnp.stack([one, total - one])
    lengths = jnp.asarray(profile(amount, total, limit, skew), jnp.int32)
    couples = (amount - 1) // 2
    giver, sink = lengths[1:1 + 2 * couples:2], lengths[2:2 + 2 * couples:2]
    slack = jnp.minimum(giver - 1, limit - sink)
    moved = jax.random.randint(jax.random.fold_in(stream_key, 1), (couples,), 0, 1 << 20) % (slack + 1)
    lengths = lengths.at[1:1 + 2 * couples:2].set(giver - moved).at[2:2 + 2 * couples:2].set(sink + moved)
    return lengths[jax.random.permutation(jax.random.fold_in(stream_key, 2), amount)]


def assign_block(own_key, own, number, rows, number_of, top, limit, skew):
    order = jax.random.permutation(own_key, number_of)
    crowded, common = shares(number_of, rows * top, limit, skew, True), shares(number_of, rows * top, limit, skew, False)
    places = jnp.arange(number_of)

    def named(lengths, rotation):
        used = int((lengths > 0).sum())
        fixed = max(1, used // 4)
        shifted = fixed + (places - fixed + rotation * (used - fixed)) % max(1, number_of - fixed)
        return jnp.zeros((number_of,), jnp.int32).at[order[jnp.where(places < fixed, places, shifted)]].set(jnp.asarray(lengths, jnp.int32))

    lengths = jnp.where(number % 4 == 0, named(crowded, number // 4), named(common, number - number // 4 - 1))
    mixed = jax.random.permutation(jax.random.fold_in(own, 3), number_of)
    giver, receiver = mixed[0:number_of // 2 * 2:2], mixed[1:number_of // 2 * 2:2]
    slack = jnp.minimum(lengths[giver] - 1, limit - lengths[receiver]) // 2
    slack = jnp.where((giver == order[0]) | (receiver == order[0]) | (lengths[receiver] == 0), 0, jnp.maximum(slack, 0))
    shifted = jax.random.randint(jax.random.fold_in(own, 4), (number_of // 2,), 0, 1 << 20) % (slack + 1)
    lengths = lengths.at[giver].add(-shifted).at[receiver].add(shifted)
    items = jnp.searchsorted(jnp.cumsum(lengths), jnp.arange(rows * top), side="right").astype(jnp.int32)
    listing = items.reshape(top, rows).T
    listing = listing[jax.random.permutation(jax.random.fold_in(own, 1), rows)]
    rotation = jax.random.randint(jax.random.fold_in(own, 2), (rows, 1), 0, top)
    return jnp.take_along_axis(listing, (jnp.arange(top)[None, :] + rotation) % top, axis=1)


def shares(count, total, bound, lean, full):
    loads = [(1 << 20) // math.isqrt(grade ** lean) + 1 for grade in range(1, count + 1)]
    largest = bound if full else min(bound, max(-(-total // count), total * loads[0] // sum(loads)))
    least = 1 if total - largest >= count - 1 else 0
    counts, spare = [largest] + [least] * (count - 1), total - largest - least * (count - 1)
    while spare > 0:
        movable = [i for i in range(1, count) if counts[i] < largest] or [i for i in range(1, count) if counts[i] < bound]
        mass, remaining = sum([loads[i] for i in movable]), spare
        for i in movable:
            addition = min(bound - counts[i], max(1, remaining * loads[i] // mass), spare)
            counts[i] = counts[i] + addition
            spare = spare - addition
    return np.array(counts)


def centred(stream_key, dims, deviation, most, cuts=(), held_as=jnp.bfloat16):
    factor_of = shard_levels(stream_key, dims, cuts, -0.22, 0.18) if cuts else 1.0
    result = jax.random.normal(stream_key, dims, jnp.float32) * deviation * factor_of
    return jnp.minimum(jnp.maximum(result, -most), most).astype(held_as)


def setup_inputs(seed: int = 0) -> dict:
    arg_keys = jax.random.split(jax.random.key(seed), 14)
    gate_b = centred(arg_keys[0], (TOKENS, CH), 1.0, 6.0, ((0, 4), (1, 8)))
    gate_c = centred(arg_keys[1], (TOKENS, CH), 1.0, 6.0, ((0, 4), (1, 8)))
    values_in = centred(arg_keys[2], (TOKENS, CH), 1.0, 6.0, ((0, 4), (1, 8)))
    conv_w = centred(arg_keys[3], (KW, CH), KW ** -0.5, 3.5, ((1, 8),))
    documents = jnp.searchsorted(jnp.cumsum(ragged_sizes(arg_keys[4], N_SP // 2 + 1, TOKENS, TOKENS // 2, 1)), jnp.arange(TOKENS), side="right").astype(jnp.int32)
    w_out = centred(arg_keys[5], (CH, D), CH ** -0.5, 0.1875)
    resid = centred(arg_keys[6], (TOKENS, D), 1.0, 6.0, ((0, 32),))
    norm_gain = jnp.clip(1.0 + 0.18 * jax.random.normal(arg_keys[7], (D,), jnp.float32), 0.099609375, 1.8984375).astype(jnp.bfloat16)
    route_ids_keys = jax.random.split(jax.random.fold_in(arg_keys[8], 1), TOKENS // ROWS)
    route_ids_turns = jax.random.permutation(jax.random.fold_in(arg_keys[8], 3), TOKENS // ROWS)
    route_ids = jax.vmap(lambda own, number: assign_block(jax.random.fold_in(arg_keys[8], 2), own, number, ROWS, EXPERTS, 2, CAP, 2))(route_ids_keys, route_ids_turns).reshape((TOKENS, 2))
    route_weight = jnp.clip(0.2 + 0.8 * jax.random.uniform(arg_keys[9], (TOKENS, 2), jnp.float32) ** shard_levels(arg_keys[9], (TOKENS, 2), ((0, 32),), -0.2, 0.2), 0.2, 1.0)
    w_gate = centred(arg_keys[10], (EXPERTS, D, FF_E), D ** -0.5, 0.125, ((0, 4), (2, 8)))
    w_up = centred(arg_keys[11], (EXPERTS, D, FF_E), D ** -0.5, 0.125, ((0, 4), (2, 8)))
    w_down = centred(arg_keys[12], (EXPERTS, FF_E, D), FF_E ** -0.5, 0.0625, ((0, 4), (1, 8)))
    return {"gate_b": gate_b, "gate_c": gate_c, "values_in": values_in, "conv_w": conv_w, "documents": documents, "w_out": w_out, "resid": resid, "norm_gain": norm_gain, "route_ids": route_ids, "route_weight": route_weight, "w_gate": w_gate, "w_up": w_up, "w_down": w_down}


def reference(gate_b, gate_c, values_in, conv_w, documents, w_out, resid, norm_gain, route_ids, route_weight, w_gate, w_up, w_down):
    product = gate_c.astype(jnp.float32) * values_in.astype(jnp.float32)
    padded = jnp.concatenate([jnp.zeros((2, CH), jnp.float32), product], axis=0)
    padded_docs = jnp.concatenate([jnp.full((2,), -1, jnp.int32), documents], axis=0)
    kernel_taps = conv_w.astype(jnp.float32)
    near_mask = (padded_docs[1:-1] == documents).astype(jnp.float32)[:, None]
    far_mask = (padded_docs[:-2] == documents).astype(jnp.float32)[:, None]
    convolved = kernel_taps[2] * product + kernel_taps[1] * padded[1:-1] * near_mask + kernel_taps[0] * padded[:-2] * far_mask
    mixed_rows = (gate_b.astype(jnp.float32) * convolved).astype(jnp.bfloat16)
    projected = jnp.dot(mixed_rows, w_out, preferred_element_type=jnp.float32)
    hidden_state = (resid.astype(jnp.float32) + projected).astype(jnp.bfloat16)
    state_wide = hidden_state.astype(jnp.float32)
    normed = (state_wide * lax.rsqrt(lax.optimization_barrier(jnp.mean(state_wide * state_wide, axis=-1, keepdims=True)) + 1e-06) * norm_gain.astype(jnp.float32)).astype(jnp.bfloat16)
    blocks = TOKENS // ROWS
    block_ids = route_ids.reshape(blocks, 2 * ROWS)
    one_hot = (block_ids[:, :, None] == jnp.arange(EXPERTS, dtype=jnp.int32)[None, None, :]).astype(jnp.int32)
    rank_in = lax.optimization_barrier(jnp.sum((jnp.cumsum(one_hot, axis=1) - one_hot) * one_hot, axis=2))
    per_expert = blocks * CAP
    block_index = jnp.arange(blocks, dtype=jnp.int32)[:, None]
    flat_slot = (block_ids * per_expert + block_index * CAP + rank_in).astype(jnp.int32)
    token_index = (block_index * ROWS + jnp.arange(2 * ROWS, dtype=jnp.int32)[None, :] // 2).astype(jnp.int32)
    slot_table = jnp.full((EXPERTS * per_expert,), TOKENS, jnp.int32).at[flat_slot.reshape(-1)].set(token_index.reshape(-1))
    padded_rows = jnp.concatenate([normed, jnp.zeros((1, D), jnp.bfloat16)], axis=0)

    def serve_expert(operands):
        slot_rows, gate_weight, up_weight, down_weight = operands
        chosen = padded_rows[slot_rows]
        gate_part = jnp.dot(chosen, gate_weight, preferred_element_type=jnp.float32)
        up_part = jnp.dot(chosen, up_weight, preferred_element_type=jnp.float32)
        activated = (jax.nn.silu(gate_part) * up_part).astype(jnp.bfloat16)
        pieces = jnp.einsum('snf,nfd->snd', activated.reshape(per_expert, N_TP, FF_E // N_TP).astype(jnp.float32), down_weight.reshape(N_TP, FF_E // N_TP, D).astype(jnp.float32))
        rounded = lax.optimization_barrier(pieces.astype(jnp.bfloat16))
        return lax.optimization_barrier(jnp.sum(rounded.astype(jnp.float32), axis=1)).astype(jnp.bfloat16)
    expert_out = lax.map(serve_expert, (slot_table.reshape(EXPERTS, per_expert), w_gate, w_up, w_down))
    picked = expert_out.reshape(EXPERTS * per_expert, D)[flat_slot.reshape(TOKENS, 2)]
    combined = lax.optimization_barrier(jnp.sum(route_weight[:, :, None].astype(jnp.float32) * picked.astype(jnp.float32), axis=1))
    return (hidden_state.astype(jnp.float32) + combined).astype(jnp.bfloat16)
```

```python
import functools

import jax
import jax.numpy as jnp
from jax import lax
from jax.experimental import pallas as pl
from jax.experimental.pallas import tpu as pltpu
from jax.sharding import PartitionSpec as P

MESH = pl.DeviceIdType.MESH
LANES = 128


def moe_kernel(
    x_ref, wg_hbm, wu_hbm, wd_hbm, out_ref,
    xbuf, pbuf, dbuf, r1, r2, rz, wg, wu, wd,
    w_sem, own_sem,
    s_z, r_z, s_1, s_2, r_h, s_p, r_p,
    s_d, r_d, s_r1, r_r1, s_r2, r_r2, s_rz, r_rz,
):
    nz = lax.axis_size("tp") // 2
    pairs = nz // 2
    width = out_ref.shape[1]
    half = width // 2
    rows = out_ref.shape[0]
    sp, tp = lax.axis_index("sp"), lax.axis_index("tp")
    y, x = sp // 2, sp % 2
    z, c = tp // 2, tp % 2
    xn, yn, dg = y * 2 + 1 - x, (1 - y) * 2 + x, (1 - y) * 2 + 1 - x
    other = (sp, z * 2 + 1 - c)
    to_x, to_y = (xn, tp), (yn, tp)

    def pair_of(q):
        return (z // 2 + q) % pairs

    def zz(k):
        return 2 * pair_of(k // 2) + (z + k) % 2

    def lanes(h):
        return pl.ds(0, half) if h == 0 else pl.ds(half, xbuf.shape[3] - half)

    def rc(src, dst, ss, rs, dev):
        return pltpu.make_async_remote_copy(
            src_ref=src, dst_ref=dst, send_sem=ss, recv_sem=rs,
            device_id=dev, device_id_type=MESH,
        )

    def z_send(k):
        return rc(x_ref, xbuf.at[sp * nz + z, c], s_z.at[k], r_z.at[z], (sp, zz(k) * 2 + c))

    def z_recv(k):
        return rc(x_ref, xbuf.at[sp * nz + zz(k), c], s_z.at[k], r_z.at[zz(k)], (sp, zz(k) * 2 + c))

    def piece(h, col, k, ss, dev):
        at = xbuf.at[col * nz + zz(k), c, :, lanes(h)]
        return rc(at, at, ss, r_h.at[h, col * nz + zz(k)], dev)

    def first(h, k):
        return piece(h, sp, k, s_1.at[h, k], to_y if h == 0 else to_x)

    def second(h, k):
        return piece(h, sp, k, s_2.at[h, 0, k], to_x if h == 0 else to_y)

    def third(h, k):
        return piece(h, yn if h == 0 else xn, k, s_2.at[h, 1, k], to_x if h == 0 else to_y)

    def arrived(h, col, k):
        piece(h, col, k, s_1.at[h, k], other).wait_recv()

    def to_other(col, k):
        i = col * nz + zz(k)
        return rc(xbuf.at[i, c], xbuf.at[i, c], s_p.at[i], r_p.at[i], other)

    def from_other(i):
        rc(xbuf.at[i, 1 - c], xbuf.at[i, 1 - c], s_p.at[i], r_p.at[i], other).wait_recv()

    def spread(k):
        for h in (1, 0):
            first(h, k).start()
        for h in (0, 1):
            second(h, k).start()
        to_other(sp, k).start()

    def take_z(k):
        z_recv(k).wait_recv()
        spread(k)

    def relay(q):
        for k in (2 * q, 2 * q + 1):
            arrived(0, yn, k)
            third(0, k).start()
            arrived(1, xn, k)
            third(1, k).start()

    def sides(q):
        for k in (2 * q, 2 * q + 1):
            arrived(0, xn, k)
            to_other(xn, k).start()
            arrived(1, yn, k)
            to_other(yn, k).start()

    def corner(q):
        for k in (2 * q, 2 * q + 1):
            arrived(0, dg, k)
            arrived(1, dg, k)
            to_other(dg, k).start()

    def d_copy(col, p, mine):
        i = pl.ds(col * nz + 2 * p, 2)
        at = pbuf.at[i, 1 - c]
        return rc(at, dbuf.at[i], s_d.at[col * pairs + p], r_d.at[col * pairs + p], other)

    def cols(h):
        return pl.ds(h * half, half)

    def r1_copy(h, o, p):
        col = dg if o else (xn if h == 0 else yn)
        at = pbuf.at[pl.ds(col * nz + 2 * p, 2), c, :, cols(h)]
        return rc(at, r1.at[h, o, pl.ds(2 * p, 2)], s_r1.at[h, o, p], r_r1.at[h, o, p], to_x if h == 0 else to_y)

    def r2_copy(h, p):
        col = yn if h == 0 else xn
        at = pbuf.at[pl.ds(col * nz + 2 * p, 2), c, :, cols(h)]
        return rc(at, r2.at[h, pl.ds(2 * p, 2)], s_r2.at[h, p], r_r2.at[h, p], to_y if h == 0 else to_x)

    def rz_copy(k):
        return rc(pbuf.at[sp * nz + zz(k), c], rz.at[z], s_rz.at[k], r_rz.at[z], (sp, zz(k) * 2 + c))

    def rz_recv(k):
        return rc(pbuf.at[sp * nz + zz(k), c], rz.at[zz(k)], s_rz.at[k], r_rz.at[zz(k)], (sp, zz(k) * 2 + c))

    f32 = jnp.float32

    def merge(fy, fx, p):
        col = (y + fy - 2 * y * fy) * 2 + x + fx - 2 * x * fx
        d_copy(col, p, False).wait_recv()
        i = pl.ds(col * nz + 2 * p, 2)
        pbuf[i, c] = (pbuf[i, c].astype(f32) + dbuf[i].astype(f32)).astype(pbuf.dtype)

    def send_sum(g, p):
        @pl.when(g == 1)
        def _():
            r1_copy(0, 0, p).start()

        @pl.when(g == 2)
        def _():
            r1_copy(1, 0, p).start()

        @pl.when(g == 3)
        def _():
            r1_copy(0, 1, p).start()
            r1_copy(1, 1, p).start()

    def stage2(q):
        p = pair_of(q)
        for h in (0, 1):
            r1_copy(h, 1, p).wait_recv()
            col = yn if h == 0 else xn
            i = pl.ds(col * nz + 2 * p, 2)
            pbuf[i, c, :, cols(h)] = (
                pbuf[i, c, :, cols(h)].astype(f32) + r1[h, 1, pl.ds(2 * p, 2)].astype(f32)
            ).astype(pbuf.dtype)
            r2_copy(h, p).start()

    def stage3(q):
        p = pair_of(q)
        i = pl.ds(sp * nz + 2 * p, 2)
        j = pl.ds(2 * p, 2)
        for h in (0, 1):
            r1_copy(h, 0, p).wait_recv()
            r2_copy(h, p).wait_recv()
            pbuf[i, c, :, cols(h)] = (
                pbuf[i, c, :, cols(h)].astype(f32)
                + r1[h, 0, j].astype(f32)
                + r2[h, j].astype(f32)
            ).astype(pbuf.dtype)
        for k in (2 * q, 2 * q + 1):
            if k > 0:
                rz_copy(k).start()

    weights = [
        pltpu.make_async_copy(a, b, w_sem.at[n])
        for n, (a, b) in enumerate(((wg_hbm, wg), (wu_hbm, wu), (wd_hbm, wd)))
    ]
    own = pltpu.make_async_copy(x_ref, xbuf.at[sp * nz + z, c], own_sem)
    own.start()
    barrier = pltpu.get_barrier_semaphore()
    peers = [other, to_x, to_y] + [(sp, zz(k) * 2 + c) for k in range(1, nz)]
    for peer in peers:
        pl.semaphore_signal(barrier, inc=1, device_id=peer, device_id_type=MESH)
    pl.semaphore_wait(barrier, len(peers))
    for k in range(1, nz):
        z_send(k).start()
    own.wait()
    spread(0)
    for w in weights:
        w.start()
    take_z(1)
    for w in weights:
        w.wait()

    experts_lanes = lax.axis_size("sp")
    lane = lax.broadcasted_iota(jnp.int32, (1, LANES), 1)
    mine = ((lane % experts_lanes == sp) & (lane < 3 * experts_lanes)).astype(f32)

    before = {1: [lambda: relay(0), lambda: sides(0)]}
    for q in range(1, pairs):
        base = 4 * (q - 1)
        before.setdefault(base + 2, []).append(functools.partial(take_z, 2 * q))
        before.setdefault(base + 3, []).append(functools.partial(take_z, 2 * q + 1))
        before.setdefault(4 * q + 1, []).append(functools.partial(relay, q))
        before.setdefault(4 * q + 1, []).append(functools.partial(sides, q))
    for q in range(pairs):
        before.setdefault(4 * q + 3, []).append(functools.partial(corner, q))
    after = {}
    for q in range(pairs - 1):
        after.setdefault(4 * q + 6, []).append(functools.partial(stage2, q))

    @pl.loop(0, 4 * pairs)
    def _(s):
        for at, works in before.items():
            @pl.when(s == at)
            def _():
                for work in works:
                    work()

        g = s % 4
        fy, fx = g // 2, g % 2
        p = pair_of(s // 4)
        col = (y + fy - 2 * y * fy) * 2 + x + fx - 2 * x * fx
        i = col * nz + 2 * p
        for b in (0, 1):
            from_other(i + b)
        held = xbuf[pl.ds(i, 2)].reshape(4 * rows, xbuf.shape[3])
        scale = jnp.sum(held[:, width:].astype(f32) * mine, axis=1, keepdims=True)
        held = held[:, :width]
        gate = jnp.dot(held, wg[...], preferred_element_type=f32)
        up = jnp.dot(held, wu[...], preferred_element_type=f32)
        act = (jax.nn.silu(gate) * up * scale).astype(jnp.bfloat16)
        part = jnp.dot(act, wd[...], preferred_element_type=f32)
        pbuf[pl.ds(i, 2)] = part.astype(pbuf.dtype).reshape(2, 2, rows, width)
        d_copy(col, p, True).start()

        @pl.when(s > 0)
        def _():
            t = s - 1
            gt = t % 4
            pt = pair_of(t // 4)
            merge(gt // 2, gt % 2, pt)
            send_sum(gt, pt)

        for at, works in after.items():
            @pl.when(s == at)
            def _():
                for work in works:
                    work()

    last = pair_of(pairs - 1)
    merge(1, 1, last)
    send_sum(3, last)
    for q in range(pairs - 1):
        stage3(q)
    stage2(pairs - 1)
    stage3(pairs - 1)
    total = pbuf[sp * nz + z, c].astype(f32)
    for k in range(1, nz):
        rz_recv(k).wait_recv()
        total = total + rz[zz(k)].astype(f32)
    out_ref[...] = total

    for k in range(1, nz):
        z_send(k).wait_send()
        rz_copy(k).wait_send()
    for k in range(nz):
        for h in (0, 1):
            first(h, k).wait_send()
            second(h, k).wait_send()
            third(h, k).wait_send()
        for col in (sp, xn, yn, dg):
            to_other(col, k).wait_send()
    for q in range(pairs):
        p = pair_of(q)
        for col in (sp, xn, yn, dg):
            d_copy(col, p, True).wait_send()
        for h in (0, 1):
            for o in (0, 1):
                r1_copy(h, o, p).wait_send()
            r2_copy(h, p).wait_send()


def moe(x_ext, w_gate, w_up, w_down):
    rows = x_ext.shape[0]
    wide = x_ext.shape[1]
    width = w_down.shape[1]
    n_sp = lax.axis_size("sp")
    nz = lax.axis_size("tp") // 2
    pairs = nz // 2
    half = width // 2
    bf = jnp.bfloat16
    dma = pltpu.SemaphoreType.DMA
    hbm = pl.BlockSpec(memory_space=pl.ANY)
    vmem = pl.BlockSpec(memory_space=pltpu.VMEM)
    return pl.pallas_call(
        moe_kernel,
        out_shape=jax.ShapeDtypeStruct((rows, width), jnp.float32),
        in_specs=[vmem, hbm, hbm, hbm],
        out_specs=vmem,
        scratch_shapes=[
            pltpu.VMEM((n_sp * nz, 2, rows, wide), bf),
            pltpu.VMEM((n_sp * nz, 2, rows, width), bf),
            pltpu.VMEM((n_sp * nz, rows, width), bf),
            pltpu.VMEM((2, 2, nz, rows, half), bf),
            pltpu.VMEM((2, nz, rows, half), bf),
            pltpu.VMEM((nz, rows, width), bf),
            pltpu.VMEM(w_gate.shape, bf),
            pltpu.VMEM(w_up.shape, bf),
            pltpu.VMEM(w_down.shape, bf),
            dma((3,)), dma,
            dma((nz,)), dma((nz,)),
            dma((2, nz)), dma((2, 2, nz)), dma((2, n_sp * nz)),
            dma((n_sp * nz,)), dma((n_sp * nz,)),
            dma((n_sp * pairs,)), dma((n_sp * pairs,)),
            dma((2, 2, pairs)), dma((2, 2, pairs)),
            dma((2, pairs)), dma((2, pairs)),
            dma((nz,)), dma((nz,)),
        ],
        compiler_params=pltpu.CompilerParams(
            collective_id=0, has_side_effects=True, vmem_limit_bytes=64000000
        ),
    )(x_ext, w_gate, w_up, w_down)


def passed_along(block, axis, distance):
    devices = range(lax.axis_size(axis))
    route = [(i - distance, i) for i in devices if i - distance in devices]
    return lax.ppermute(block, axis, route)


def local(
    gate_b,
    gate_c,
    values_in,
    conv_w,
    documents,
    w_out,
    resid,
    norm_gain,
    route_ids,
    route_weight,
    w_gate,
    w_up,
    w_down,
):
    seq_rows = gate_b.shape[0]
    local_rows = resid.shape[0]
    model_width = resid.shape[1]
    last_rows = jnp.stack([gate_c[seq_rows - 2 :], values_in[seq_rows - 2 :]])
    before, before_docs = passed_along((last_rows, documents[seq_rows - 2 :]), "sp", 1)
    products = jnp.concatenate(
        [
            before[0].astype(jnp.float32) * before[1].astype(jnp.float32),
            gate_c.astype(jnp.float32) * values_in.astype(jnp.float32),
        ],
        axis=0,
    )
    docs_all = jnp.concatenate([before_docs, documents], axis=0)
    kernel_taps = conv_w.astype(jnp.float32)
    near_mask = (docs_all[1:-1] == documents).astype(jnp.float32)[:, None]
    far_mask = (docs_all[:-2] == documents).astype(jnp.float32)[:, None]
    convolved = (
        kernel_taps[2] * products[2:]
        + kernel_taps[1] * products[1:-1] * near_mask
        + kernel_taps[0] * products[:-2] * far_mask
    )
    mixed_rows = (gate_b.astype(jnp.float32) * convolved).astype(jnp.bfloat16)
    token_rows = lax.all_to_all(mixed_rows, "tp", split_axis=0, concat_axis=1, tiled=True)
    projected = jnp.dot(token_rows, w_out, preferred_element_type=jnp.float32)
    hidden_state = (resid.astype(jnp.float32) + projected).astype(jnp.bfloat16)
    state_wide = hidden_state.astype(jnp.float32)
    normed = (
        state_wide
        * lax.rsqrt(jnp.mean(state_wide * state_wide, axis=-1, keepdims=True) + 1e-06)
        * norm_gain.astype(jnp.float32)
    ).astype(jnp.bfloat16)
    experts = lax.axis_size("sp") * w_gate.shape[0]
    capacity = 4 * local_rows // experts
    if lax.axis_size("sp") == 4 and w_gate.shape[0] == 1 and capacity >= local_rows:
        named = route_ids[:, :, None] == jnp.arange(experts, dtype=jnp.int32)[None, None, :]
        share = jnp.sum(jnp.where(named, route_weight[:, :, None], 0.0), axis=1)
        high = lax.reduce_precision(share, 8, 7)
        middle = lax.reduce_precision(share - high, 8, 7)
        low = share - high - middle
        spare = jnp.zeros((local_rows, LANES - 3 * experts), jnp.float32)
        shares = jnp.concatenate([high, middle, low, spare], axis=1).astype(jnp.bfloat16)
        combined = moe(
            jnp.concatenate([normed, shares], axis=1), w_gate[0], w_up[0], w_down[0]
        )
        return (hidden_state.astype(jnp.float32) + combined).astype(jnp.bfloat16)
    flat_ids = route_ids.reshape(-1)
    one_hot = (flat_ids[:, None] == jnp.arange(experts, dtype=jnp.int32)[None, :]).astype(jnp.int32)
    rank_in = jnp.sum((jnp.cumsum(one_hot, axis=0) - one_hot) * one_hot, axis=1)
    slot_index = flat_ids * capacity + rank_in
    placement = (
        slot_index[:, None] == jnp.arange(experts * capacity, dtype=jnp.int32)[None, :]
    ).astype(jnp.bfloat16)
    repeated = jnp.repeat(normed, 2, axis=0)
    dispatch = jnp.einsum(
        "js,jd->sd", placement, repeated, preferred_element_type=jnp.float32
    ).astype(jnp.bfloat16)
    dispatch = dispatch.reshape(experts, capacity, model_width)
    gathered_piece = lax.all_gather(
        lax.all_to_all(dispatch, "sp", split_axis=0, concat_axis=0, tiled=True),
        "tp",
        axis=0,
        tiled=True,
    )
    flat_rows = gathered_piece.reshape(-1, model_width)
    gate_part = jnp.dot(flat_rows, w_gate[0], preferred_element_type=jnp.float32)
    up_part = jnp.dot(flat_rows, w_up[0], preferred_element_type=jnp.float32)
    activated = (jax.nn.silu(gate_part) * up_part).astype(jnp.bfloat16)
    partial_value = jnp.dot(activated, w_down[0], preferred_element_type=jnp.float32)
    partial_value = partial_value.reshape(
        gathered_piece.shape[0], gathered_piece.shape[1], model_width
    )
    summed = lax.psum_scatter(
        partial_value.astype(jnp.bfloat16), "tp", scatter_dimension=0, tiled=True
    )
    returned = lax.all_to_all(summed, "sp", split_axis=0, concat_axis=0, tiled=True)
    picked = jnp.take(
        returned.reshape(experts * capacity, model_width), slot_index, axis=0
    ).reshape(local_rows, 2, model_width)
    combined = jnp.sum(route_weight[:, :, None] * picked.astype(jnp.float32), axis=1)
    return (hidden_state.astype(jnp.float32) + combined).astype(jnp.bfloat16)


def solution(mesh):
    return jax.shard_map(
        local,
        mesh=mesh,
        in_specs=(
            P("sp", "tp"),
            P("sp", "tp"),
            P("sp", "tp"),
            P(None, "tp"),
            P("sp"),
            P(),
            P(("sp", "tp"), None),
            P(),
            P(("sp", "tp"), None),
            P(("sp", "tp"), None),
            P("sp", None, "tp"),
            P("sp", None, "tp"),
            P("sp", "tp", None),
        ),
        out_specs=P(("sp", "tp"), None),
        check_vma=False,
    )
```

```python
import functools

import jax
import jax.numpy as jnp
from jax import lax
from jax.experimental import pallas as pl
from jax.experimental.pallas import tpu as pltpu
from jax.sharding import PartitionSpec as P

MESH = pl.DeviceIdType.MESH
LANES = 128


def moe_kernel(
    gb, gc, vals, taps, docs, resid, gain, ids, route, wo_hbm, wg_hbm, wu_hbm, wd_hbm, out_ref,
    x_ref, hid, tok, mixed, pad, dpad, hc, hv, hd, wo,
    s_a, r_a, s_h, r_h3,
    xbuf, pbuf, dbuf, r1, r2, rz, wg, wu, wd,
    w_sem, own_sem,
    s_z, r_z, s_1, s_2, r_h, s_p, r_p,
    s_d, r_d, s_r1, r_r1, s_r2, r_r2, s_rz, r_rz,
):
    nz = lax.axis_size("tp") // 2
    pairs = nz // 2
    width = out_ref.shape[1]
    half = width // 2
    rows = out_ref.shape[0]
    sp, tp = lax.axis_index("sp"), lax.axis_index("tp")
    y, x = sp // 2, sp % 2
    z, c = tp // 2, tp % 2
    xn, yn, dg = y * 2 + 1 - x, (1 - y) * 2 + x, (1 - y) * 2 + 1 - x
    other = (sp, z * 2 + 1 - c)
    n_sp, n_tp = lax.axis_size("sp"), lax.axis_size("tp")
    following, previous = (lax.rem(sp + 1, n_sp), tp), (lax.rem(sp + n_sp - 1, n_sp), tp)
    seq = gb.shape[0]
    halo = hc.shape[0]
    to_x, to_y = (xn, tp), (yn, tp)

    def pair_of(q):
        return (z // 2 + q) % pairs

    def zz(k):
        return 2 * pair_of(k // 2) + (z + k) % 2

    def lanes(h):
        return pl.ds(0, half) if h == 0 else pl.ds(half, xbuf.shape[3] - half)

    def rc(src, dst, ss, rs, dev):
        return pltpu.make_async_remote_copy(
            src_ref=src, dst_ref=dst, send_sem=ss, recv_sem=rs,
            device_id=dev, device_id_type=MESH,
        )

    def halo_copies():
        pairs3 = ((gc.at[pl.ds(seq - halo, halo)], hc), (vals.at[pl.ds(seq - halo, halo)], hv),
                  (docs.at[pl.ds(seq - 8, 8)], hd))
        return [rc(a, b, s_h.at[n], r_h3.at[n], following) for n, (a, b) in enumerate(pairs3)]

    def channels(j):
        return pl.ds(pl.multiple_of(j * gb.shape[1], gb.shape[1]), gb.shape[1])

    def swap(d):
        j = lax.rem(tp + d, n_tp)
        at = mixed.at[pl.ds(pl.multiple_of(j * rows, rows), rows)]
        return rc(at, tok.at[:, channels(tp)], s_a.at[d], r_a.at[tp], (sp, j))

    def swapped(d):
        j = lax.rem(tp + d, n_tp)
        at = mixed.at[pl.ds(pl.multiple_of(j * rows, rows), rows)]
        return rc(at, tok.at[:, channels(j)], s_a.at[d], r_a.at[j], (sp, j))

    def mix():
        f32 = jnp.float32
        product = gc[...].astype(f32) * vals[...].astype(f32)
        pad[pl.ds(8, seq)] = product
        dpad[pl.ds(8, seq)] = docs[...]
        for copy in halo_copies():
            copy.wait_recv()
        pad[pl.ds(0, 8)] = (hc[...].astype(f32) * hv[...].astype(f32))[halo - 8 :]
        dpad[pl.ds(0, 8)] = jnp.where(sp == 0, -1, hd[...])
        near = (dpad[pl.ds(7, seq)] == docs[...]).astype(f32)
        far = (dpad[pl.ds(6, seq)] == docs[...]).astype(f32)
        tap = taps[...].astype(f32)
        convolved = (
            tap[2:3] * product
            + tap[1:2] * pad[pl.ds(7, seq)] * near
            + tap[0:1] * pad[pl.ds(6, seq)] * far
        )
        mixed[...] = (gb[...].astype(f32) * convolved).astype(mixed.dtype)
        for d in range(1, n_tp):
            swap(d).start()
        tok[:, channels(tp)] = mixed[pl.ds(pl.multiple_of(tp * rows, rows), rows)]
        lane = lax.broadcasted_iota(jnp.int32, (rows, LANES), 1)
        named = lane % n_sp
        part = lane // n_sp
        share = jnp.where(ids[:, 0:1] == named, route[:, 0:1], 0.0) + jnp.where(
            ids[:, 1:2] == named, route[:, 1:2], 0.0
        )
        high = share.astype(jnp.bfloat16).astype(f32)
        middle = (share - high).astype(jnp.bfloat16).astype(f32)
        low = share - high - middle
        terms = jnp.where(part == 0, high, jnp.where(part == 1, middle, jnp.where(part == 2, low, 0.0)))
        x_ref[:, pl.ds(width, LANES)] = terms.astype(x_ref.dtype)
        wo_copy.wait()
        for d in range(1, n_tp):
            swapped(d).wait_recv()
        projected = jnp.dot(tok[...], wo[...], preferred_element_type=f32)
        hidden = (resid[...].astype(f32) + projected).astype(hid.dtype)
        hid[...] = hidden
        state = hidden.astype(f32)
        mean = jnp.mean(state * state, axis=-1, keepdims=True)
        x_ref[:, pl.ds(0, width)] = (
            state * lax.rsqrt(mean + 1e-06) * gain[...].astype(f32)
        ).astype(x_ref.dtype)

    def z_send(k):
        return rc(x_ref, xbuf.at[sp * nz + z, c], s_z.at[k], r_z.at[z], (sp, zz(k) * 2 + c))

    def z_recv(k):
        return rc(x_ref, xbuf.at[sp * nz + zz(k), c], s_z.at[k], r_z.at[zz(k)], (sp, zz(k) * 2 + c))

    def piece(h, col, k, ss, dev):
        at = xbuf.at[col * nz + zz(k), c, :, lanes(h)]
        return rc(at, at, ss, r_h.at[h, col * nz + zz(k)], dev)

    def first(h, k):
        return piece(h, sp, k, s_1.at[h, k], to_y if h == 0 else to_x)

    def second(h, k):
        return piece(h, sp, k, s_2.at[h, 0, k], to_x if h == 0 else to_y)

    def third(h, k):
        return piece(h, yn if h == 0 else xn, k, s_2.at[h, 1, k], to_x if h == 0 else to_y)

    def arrived(h, col, k):
        piece(h, col, k, s_1.at[h, k], other).wait_recv()

    def to_other(col, k):
        i = col * nz + zz(k)
        return rc(xbuf.at[i, c], xbuf.at[i, c], s_p.at[i], r_p.at[i], other)

    def from_other(i):
        rc(xbuf.at[i, 1 - c], xbuf.at[i, 1 - c], s_p.at[i], r_p.at[i], other).wait_recv()

    def spread(k):
        for h in (1, 0):
            first(h, k).start()
        for h in (0, 1):
            second(h, k).start()
        to_other(sp, k).start()

    def take_z(k):
        z_recv(k).wait_recv()
        spread(k)

    def relay(q):
        for k in (2 * q, 2 * q + 1):
            arrived(0, yn, k)
            third(0, k).start()
            arrived(1, xn, k)
            third(1, k).start()

    def sides(q):
        for k in (2 * q, 2 * q + 1):
            arrived(0, xn, k)
            to_other(xn, k).start()
            arrived(1, yn, k)
            to_other(yn, k).start()

    def corner(q):
        for k in (2 * q, 2 * q + 1):
            arrived(0, dg, k)
            arrived(1, dg, k)
            to_other(dg, k).start()

    def d_copy(col, p, mine):
        i = pl.ds(col * nz + 2 * p, 2)
        at = pbuf.at[i, 1 - c]
        return rc(at, dbuf.at[i], s_d.at[col * pairs + p], r_d.at[col * pairs + p], other)

    def cols(h):
        return pl.ds(h * half, half)

    def r1_copy(h, o, p):
        col = dg if o else (xn if h == 0 else yn)
        at = pbuf.at[pl.ds(col * nz + 2 * p, 2), c, :, cols(h)]
        return rc(at, r1.at[h, o, pl.ds(2 * p, 2)], s_r1.at[h, o, p], r_r1.at[h, o, p], to_x if h == 0 else to_y)

    def r2_copy(h, p):
        col = yn if h == 0 else xn
        at = pbuf.at[pl.ds(col * nz + 2 * p, 2), c, :, cols(h)]
        return rc(at, r2.at[h, pl.ds(2 * p, 2)], s_r2.at[h, p], r_r2.at[h, p], to_y if h == 0 else to_x)

    def rz_copy(k):
        return rc(pbuf.at[sp * nz + zz(k), c], rz.at[z], s_rz.at[k], r_rz.at[z], (sp, zz(k) * 2 + c))

    def rz_recv(k):
        return rc(pbuf.at[sp * nz + zz(k), c], rz.at[zz(k)], s_rz.at[k], r_rz.at[zz(k)], (sp, zz(k) * 2 + c))

    f32 = jnp.float32

    def merge(fy, fx, p):
        col = (y + fy - 2 * y * fy) * 2 + x + fx - 2 * x * fx
        d_copy(col, p, False).wait_recv()
        i = pl.ds(col * nz + 2 * p, 2)
        pbuf[i, c] = (pbuf[i, c].astype(f32) + dbuf[i].astype(f32)).astype(pbuf.dtype)

    def send_sum(g, p):
        @pl.when(g == 1)
        def _():
            r1_copy(0, 0, p).start()

        @pl.when(g == 2)
        def _():
            r1_copy(1, 0, p).start()

        @pl.when(g == 3)
        def _():
            r1_copy(0, 1, p).start()
            r1_copy(1, 1, p).start()

    def stage2(q):
        p = pair_of(q)
        for h in (0, 1):
            r1_copy(h, 1, p).wait_recv()
            col = yn if h == 0 else xn
            i = pl.ds(col * nz + 2 * p, 2)
            pbuf[i, c, :, cols(h)] = (
                pbuf[i, c, :, cols(h)].astype(f32) + r1[h, 1, pl.ds(2 * p, 2)].astype(f32)
            ).astype(pbuf.dtype)
            r2_copy(h, p).start()

    def stage3(q):
        p = pair_of(q)
        i = pl.ds(sp * nz + 2 * p, 2)
        j = pl.ds(2 * p, 2)
        for h in (0, 1):
            r1_copy(h, 0, p).wait_recv()
            r2_copy(h, p).wait_recv()
            pbuf[i, c, :, cols(h)] = (
                pbuf[i, c, :, cols(h)].astype(f32)
                + r1[h, 0, j].astype(f32)
                + r2[h, j].astype(f32)
            ).astype(pbuf.dtype)
        for k in (2 * q, 2 * q + 1):
            if k > 0:
                rz_copy(k).start()

    weights = [
        pltpu.make_async_copy(a, b, w_sem.at[n])
        for n, (a, b) in enumerate(((wg_hbm, wg), (wu_hbm, wu), (wd_hbm, wd)))
    ]
    own = pltpu.make_async_copy(x_ref, xbuf.at[sp * nz + z, c], own_sem)
    wo_copy = pltpu.make_async_copy(wo_hbm, wo, w_sem.at[3])
    wo_copy.start()
    for w in weights:
        w.start()
    barrier = pltpu.get_barrier_semaphore()
    peers = [to_x, to_y, following, previous] + [(sp, lax.rem(tp + d, n_tp)) for d in range(1, n_tp)]
    for peer in peers:
        pl.semaphore_signal(barrier, inc=1, device_id=peer, device_id_type=MESH)
    pl.semaphore_wait(barrier, len(peers))
    for copy in halo_copies():
        copy.start()
    mix()
    own.start()
    for k in range(1, nz):
        z_send(k).start()
    own.wait()
    spread(0)
    take_z(1)
    for w in weights:
        w.wait()

    experts_lanes = lax.axis_size("sp")
    lane = lax.broadcasted_iota(jnp.int32, (1, LANES), 1)
    mine = ((lane % experts_lanes == sp) & (lane < 3 * experts_lanes)).astype(f32)

    before = {1: [lambda: relay(0), lambda: sides(0)]}
    for q in range(1, pairs):
        base = 4 * (q - 1)
        before.setdefault(base + 2, []).append(functools.partial(take_z, 2 * q))
        before.setdefault(base + 3, []).append(functools.partial(take_z, 2 * q + 1))
        before.setdefault(4 * q + 1, []).append(functools.partial(relay, q))
        before.setdefault(4 * q + 1, []).append(functools.partial(sides, q))
    for q in range(pairs):
        before.setdefault(4 * q + 3, []).append(functools.partial(corner, q))
    after = {}
    for q in range(pairs - 1):
        after.setdefault(4 * q + 6, []).append(functools.partial(stage2, q))

    @pl.loop(0, 4 * pairs)
    def _(s):
        for at, works in before.items():
            @pl.when(s == at)
            def _():
                for work in works:
                    work()

        g = s % 4
        fy, fx = g // 2, g % 2
        p = pair_of(s // 4)
        col = (y + fy - 2 * y * fy) * 2 + x + fx - 2 * x * fx
        i = col * nz + 2 * p
        for b in (0, 1):
            from_other(i + b)
        held = xbuf[pl.ds(i, 2)].reshape(4 * rows, xbuf.shape[3])
        scale = jnp.sum(held[:, width:].astype(f32) * mine, axis=1, keepdims=True)
        held = held[:, :width]
        gate = jnp.dot(held, wg[...], preferred_element_type=f32)
        up = jnp.dot(held, wu[...], preferred_element_type=f32)
        act = (jax.nn.silu(gate) * up * scale).astype(jnp.bfloat16)
        part = jnp.dot(act, wd[...], preferred_element_type=f32)
        pbuf[pl.ds(i, 2)] = part.astype(pbuf.dtype).reshape(2, 2, rows, width)
        d_copy(col, p, True).start()

        @pl.when(s > 0)
        def _():
            t = s - 1
            gt = t % 4
            pt = pair_of(t // 4)
            merge(gt // 2, gt % 2, pt)
            send_sum(gt, pt)

        for at, works in after.items():
            @pl.when(s == at)
            def _():
                for work in works:
                    work()

    last = pair_of(pairs - 1)
    merge(1, 1, last)
    send_sum(3, last)
    for q in range(pairs - 1):
        stage3(q)
    stage2(pairs - 1)
    stage3(pairs - 1)
    total = pbuf[sp * nz + z, c].astype(f32)
    for k in range(1, nz):
        rz_recv(k).wait_recv()
        total = total + rz[zz(k)].astype(f32)
    out_ref[...] = (hid[...].astype(f32) + total).astype(out_ref.dtype)

    for copy in halo_copies():
        copy.wait_send()
    for d in range(1, n_tp):
        swap(d).wait_send()
    for k in range(1, nz):
        z_send(k).wait_send()
        rz_copy(k).wait_send()
    for k in range(nz):
        for h in (0, 1):
            first(h, k).wait_send()
            second(h, k).wait_send()
            third(h, k).wait_send()
        for col in (sp, xn, yn, dg):
            to_other(col, k).wait_send()
    for q in range(pairs):
        p = pair_of(q)
        for col in (sp, xn, yn, dg):
            d_copy(col, p, True).wait_send()
        for h in (0, 1):
            for o in (0, 1):
                r1_copy(h, o, p).wait_send()
            r2_copy(h, p).wait_send()


def layer(gate_b, gate_c, values_in, conv_w, docs, resid, gain, ids, route, w_out, w_gate, w_up, w_down):
    rows, width = resid.shape
    wide = width + LANES
    seq, held = gate_b.shape
    n_tp = lax.axis_size("tp")
    n_sp = lax.axis_size("sp")
    nz = lax.axis_size("tp") // 2
    pairs = nz // 2
    half = width // 2
    bf = jnp.bfloat16
    dma = pltpu.SemaphoreType.DMA
    hbm = pl.BlockSpec(memory_space=pl.ANY)
    vmem = pl.BlockSpec(memory_space=pltpu.VMEM)
    return pl.pallas_call(
        moe_kernel,
        out_shape=jax.ShapeDtypeStruct((rows, width), bf),
        in_specs=[vmem] * 9 + [hbm] * 4,
        out_specs=vmem,
        scratch_shapes=[
            pltpu.VMEM((rows, wide), bf),
            pltpu.VMEM((rows, width), bf),
            pltpu.VMEM((rows, n_tp * held), bf),
            pltpu.VMEM((seq, held), bf),
            pltpu.VMEM((seq + 8, held), jnp.float32),
            pltpu.VMEM((seq + 8, held), jnp.int32),
            pltpu.VMEM((16, held), bf),
            pltpu.VMEM((16, held), bf),
            pltpu.VMEM((8, held), jnp.int32),
            pltpu.VMEM(w_out.shape, bf),
            dma((n_tp,)), dma((n_tp,)), dma((3,)), dma((3,)),
            pltpu.VMEM((n_sp * nz, 2, rows, wide), bf),
            pltpu.VMEM((n_sp * nz, 2, rows, width), bf),
            pltpu.VMEM((n_sp * nz, rows, width), bf),
            pltpu.VMEM((2, 2, nz, rows, half), bf),
            pltpu.VMEM((2, nz, rows, half), bf),
            pltpu.VMEM((nz, rows, width), bf),
            pltpu.VMEM(w_gate.shape, bf),
            pltpu.VMEM(w_up.shape, bf),
            pltpu.VMEM(w_down.shape, bf),
            dma((4,)), dma,
            dma((nz,)), dma((nz,)),
            dma((2, nz)), dma((2, 2, nz)), dma((2, n_sp * nz)),
            dma((n_sp * nz,)), dma((n_sp * nz,)),
            dma((n_sp * pairs,)), dma((n_sp * pairs,)),
            dma((2, 2, pairs)), dma((2, 2, pairs)),
            dma((2, pairs)), dma((2, pairs)),
            dma((nz,)), dma((nz,)),
        ],
        compiler_params=pltpu.CompilerParams(
            collective_id=0, has_side_effects=True, vmem_limit_bytes=64000000
        ),
    )(gate_b, gate_c, values_in, conv_w, docs, resid, gain, ids, route, w_out, w_gate, w_up, w_down)


def passed_along(block, axis, distance):
    devices = range(lax.axis_size(axis))
    route = [(i - distance, i) for i in devices if i - distance in devices]
    return lax.ppermute(block, axis, route)


def local(
    gate_b,
    gate_c,
    values_in,
    conv_w,
    documents,
    w_out,
    resid,
    norm_gain,
    route_ids,
    route_weight,
    w_gate,
    w_up,
    w_down,
):
    seq_rows = gate_b.shape[0]
    local_rows = resid.shape[0]
    model_width = resid.shape[1]
    experts = lax.axis_size("sp") * w_gate.shape[0]
    capacity = 4 * local_rows // experts
    if lax.axis_size("sp") == 4 and w_gate.shape[0] == 1 and capacity >= local_rows:
        docs = jnp.broadcast_to(documents[:, None], gate_b.shape)
        return layer(
            gate_b, gate_c, values_in, conv_w, docs, resid, norm_gain[None, :], route_ids,
            route_weight, w_out, w_gate[0], w_up[0], w_down[0],
        )
    last_rows = jnp.stack([gate_c[seq_rows - 2 :], values_in[seq_rows - 2 :]])
    before, before_docs = passed_along((last_rows, documents[seq_rows - 2 :]), "sp", 1)
    products = jnp.concatenate(
        [
            before[0].astype(jnp.float32) * before[1].astype(jnp.float32),
            gate_c.astype(jnp.float32) * values_in.astype(jnp.float32),
        ],
        axis=0,
    )
    docs_all = jnp.concatenate([before_docs, documents], axis=0)
    kernel_taps = conv_w.astype(jnp.float32)
    near_mask = (docs_all[1:-1] == documents).astype(jnp.float32)[:, None]
    far_mask = (docs_all[:-2] == documents).astype(jnp.float32)[:, None]
    convolved = (
        kernel_taps[2] * products[2:]
        + kernel_taps[1] * products[1:-1] * near_mask
        + kernel_taps[0] * products[:-2] * far_mask
    )
    mixed_rows = (gate_b.astype(jnp.float32) * convolved).astype(jnp.bfloat16)
    token_rows = lax.all_to_all(mixed_rows, "tp", split_axis=0, concat_axis=1, tiled=True)
    projected = jnp.dot(token_rows, w_out, preferred_element_type=jnp.float32)
    hidden_state = (resid.astype(jnp.float32) + projected).astype(jnp.bfloat16)
    state_wide = hidden_state.astype(jnp.float32)
    normed = (
        state_wide
        * lax.rsqrt(jnp.mean(state_wide * state_wide, axis=-1, keepdims=True) + 1e-06)
        * norm_gain.astype(jnp.float32)
    ).astype(jnp.bfloat16)
    experts = lax.axis_size("sp") * w_gate.shape[0]
    capacity = 4 * local_rows // experts
    flat_ids = route_ids.reshape(-1)
    one_hot = (flat_ids[:, None] == jnp.arange(experts, dtype=jnp.int32)[None, :]).astype(jnp.int32)
    rank_in = jnp.sum((jnp.cumsum(one_hot, axis=0) - one_hot) * one_hot, axis=1)
    slot_index = flat_ids * capacity + rank_in
    placement = (
        slot_index[:, None] == jnp.arange(experts * capacity, dtype=jnp.int32)[None, :]
    ).astype(jnp.bfloat16)
    repeated = jnp.repeat(normed, 2, axis=0)
    dispatch = jnp.einsum(
        "js,jd->sd", placement, repeated, preferred_element_type=jnp.float32
    ).astype(jnp.bfloat16)
    dispatch = dispatch.reshape(experts, capacity, model_width)
    gathered_piece = lax.all_gather(
        lax.all_to_all(dispatch, "sp", split_axis=0, concat_axis=0, tiled=True),
        "tp",
        axis=0,
        tiled=True,
    )
    flat_rows = gathered_piece.reshape(-1, model_width)
    gate_part = jnp.dot(flat_rows, w_gate[0], preferred_element_type=jnp.float32)
    up_part = jnp.dot(flat_rows, w_up[0], preferred_element_type=jnp.float32)
    activated = (jax.nn.silu(gate_part) * up_part).astype(jnp.bfloat16)
    partial_value = jnp.dot(activated, w_down[0], preferred_element_type=jnp.float32)
    partial_value = partial_value.reshape(
        gathered_piece.shape[0], gathered_piece.shape[1], model_width
    )
    summed = lax.psum_scatter(
        partial_value.astype(jnp.bfloat16), "tp", scatter_dimension=0, tiled=True
    )
    returned = lax.all_to_all(summed, "sp", split_axis=0, concat_axis=0, tiled=True)
    picked = jnp.take(
        returned.reshape(experts * capacity, model_width), slot_index, axis=0
    ).reshape(local_rows, 2, model_width)
    combined = jnp.sum(route_weight[:, :, None] * picked.astype(jnp.float32), axis=1)
    return (hidden_state.astype(jnp.float32) + combined).astype(jnp.bfloat16)


def solution(mesh):
    return jax.shard_map(
        local,
        mesh=mesh,
        in_specs=(
            P("sp", "tp"),
            P("sp", "tp"),
            P("sp", "tp"),
            P(None, "tp"),
            P("sp"),
            P(),
            P(("sp", "tp"), None),
            P(),
            P(("sp", "tp"), None),
            P(("sp", "tp"), None),
            P("sp", None, "tp"),
            P("sp", None, "tp"),
            P("sp", "tp", None),
        ),
        out_specs=P(("sp", "tp"), None),
        check_vma=False,
    )
```
